128 devices in a mesh: kv: 16 (over z, x), tp: 8 (over y, core).
Axes of the slice: x: 4, y: 4, z: 4, core: 2. Of those that a mesh axis runs over, the one named last changes fastest.
Arguments:
- tokens: bfloat16 [64, 2048], P(None, 'kv'), may hold values from -6 to 6
- token_gain: float32 [2048], P('kv'), may hold values from 0.1 to 1.9
- w_query: bfloat16 [2048, 1536], P('kv', 'tp'), may hold values from -0.125 to 0.125
- w_down_kv: bfloat16 [2048, 512], P('kv'), may hold values from -0.125 to 0.125
- w_rope_key: bfloat16 [2048, 64], P('kv'), may hold values from -0.125 to 0.125
- latent_gain: float32 [512], replicated, may hold values from 0.1 to 1.9
- w_key_up: bfloat16 [8, 512, 128], P('tp'), may hold values from -0.25 to 0.25
- w_value_up: bfloat16 [8, 512, 128], P('tp'), may hold values from -0.25 to 0.25
- w_out: bfloat16 [1024, 2048], P('tp', 'kv'), may hold values from -0.1875 to 0.1875
- out_gain: float32 [2048], P('kv'), may hold values from 0.1 to 1.9
- cache_latent: bfloat16 [64, 8192, 512], P('tp', 'kv'), may hold values from -6 to 6
- cache_rope: bfloat16 [64, 8192, 64], P('tp', 'kv'), may hold values from -6 to 6
- lengths: int32 [64], replicated, may hold values from 1 to 8191, as said below
Outputs:
- mixed: bfloat16 [64, 2048], P(None, 'kv')
The draws below stay inside these ranges and needn't reach their ends.
Inputs may be any that keep to these rules, and one draw needn't show every extreme that they name: `lengths`: each of the 64 sequences has 1 to 8191 cached positions; some sequence has exactly 8191 and some exactly 1.
All inputs are finite; a program needn't handle non-finite values.
Results may differ from the reference program's by a relative error of at most 0.015.
Values may be sent and summed in bfloat16 or wider, within the bound.
A program may use at most 64 MiB of HBM per device.

```python
import jax
import jax.numpy as jnp
from jax import lax

D = 2048
HEADS = 8
LATENT = 512
NOPE = 128
ROPE = 64
VDIM = 128
BATCH = 64
CACHE_LEN = 8192


def draw_lengths(key, part):
    first_key, second_key = jax.random.split(jax.random.fold_in(key, 11))
    first_draw = jax.random.randint(first_key, (BATCH,), 1, CACHE_LEN)
    second_draw = jax.random.randint(second_key, (BATCH,), 1, CACHE_LEN)
    joined = jnp.minimum(first_draw, second_draw)
    joined = joined.at[0].set(CACHE_LEN - 1).at[BATCH - 1].set(1)
    return joined.astype(jnp.int32)


def block_scale(stream_key, extent, shards, least, high):
    def one(axis_at, shards_of):
        heights = jax.random.uniform(jax.random.fold_in(jax.random.fold_in(stream_key, 6), axis_at), (shards_of,), jnp.float32, least / len(shards), high / len(shards))
        return jnp.repeat(jnp.exp(heights), extent[axis_at] // shards_of).reshape((-1,) + (1,) * (len(extent) - axis_at - 1))

    gain = one(*shards[0])
    for cut in shards[1:]:
        gain = gain * one(*cut)
    return gain


def centred(stream_key, shape, spread, limit, pieces=(), kind=jnp.bfloat16):
    values = jax.random.normal(stream_key, shape, jnp.float32) * spread
    if len(pieces) > 0:
        values = block_scale(stream_key, shape, pieces, -0.22, 0.18) * values
    return jnp.clip(values, min=-limit, max=limit).astype(kind)


def setup_inputs(seed: int = 0) -> dict:
    keys = jax.random.split(jax.random.key(seed), 14)
    return {
        "tokens": centred(keys[0], (BATCH, D), 1.0, 6.0, ((1, 16),)),
        "token_gain": jnp.clip(1.0 + 0.18 * jax.random.normal(keys[1], (D,), jnp.float32), 0.1, 1.9),
        "w_query": centred(keys[2], (D, HEADS * (NOPE + ROPE)), D ** -0.5, 0.125, ((0, 16), (1, 8))),
        "w_down_kv": centred(keys[3], (D, LATENT), D ** -0.5, 0.125, ((0, 16),)),
        "w_rope_key": centred(keys[4], (D, ROPE), D ** -0.5, 0.125, ((0, 16),)),
        "latent_gain": jnp.clip(1.0 + 0.18 * jax.random.normal(keys[5], (LATENT,), jnp.float32), 0.1, 1.9),
        "w_key_up": centred(keys[6], (HEADS, LATENT, NOPE), LATENT ** -0.5, 0.25, ((0, 8),)),
        "w_value_up": centred(keys[7], (HEADS, LATENT, VDIM), LATENT ** -0.5, 0.25, ((0, 8),)),
        "w_out": centred(keys[8], (HEADS * VDIM, D), (HEADS * VDIM) ** -0.5, 0.1875, ((0, 8), (1, 16))),
        "out_gain": jnp.clip(1.0 + 0.18 * jax.random.normal(keys[9], (D,), jnp.float32), 0.1, 1.9),
        "cache_latent": centred(keys[10], (BATCH, CACHE_LEN, LATENT), 1.0, 6.0, ((0, 8), (1, 16))),
        "cache_rope": centred(keys[11], (BATCH, CACHE_LEN, ROPE), 1.0, 6.0, ((0, 8), (1, 16))),
        "lengths": draw_lengths(jax.random.fold_in(keys[13], 71), 0),
    }


EPSILON = 1e-06
NEGATIVE = -1e+30

def rotate_half(values, cosine, sine_table):
    half_width = values.shape[-1] // 2
    lower_half = values[..., :half_width]
    upper_half = values[..., half_width:]
    return jnp.concatenate([lower_half * cosine - upper_half * sine_table, upper_half * cosine + lower_half * sine_table], axis=-1)

def angle_tables(lengths, rope_width):
    inverse_freq = 1.0 / 10000.0 ** (jnp.arange(0, rope_width, 2, dtype=jnp.float32) / rope_width)
    angles = lengths.astype(jnp.float32)[:, None] * inverse_freq[None, :]
    return (jnp.cos(angles), jnp.sin(angles))

def attend_one(packed):
    query_lat, query_rot, new_latent, new_key, length, cached_lat, cached_rot = packed
    factor = (NOPE + ROPE) ** (-0.5)
    scores = (jnp.dot(query_lat, cached_lat.T, preferred_element_type=jnp.float32) + jnp.dot(query_rot, cached_rot.T, preferred_element_type=jnp.float32)) * factor
    new_score = (jnp.dot(query_lat, new_latent, preferred_element_type=jnp.float32) + jnp.dot(query_rot, new_key, preferred_element_type=jnp.float32)) * factor
    visible = jnp.arange(CACHE_LEN) < length
    top_score = jnp.maximum(lax.optimization_barrier(jnp.max(jnp.where(visible[None, :], scores, NEGATIVE), axis=1)), new_score)
    weights = jnp.where(visible[None, :], jnp.exp(scores - top_score[:, None]), jnp.float32(0.0))
    new_weight = jnp.exp(new_score - top_score)
    weight_sum = lax.optimization_barrier(jnp.sum(weights, axis=1)) + new_weight
    rounded_new = lax.optimization_barrier(new_weight.astype(jnp.bfloat16)).astype(jnp.float32)
    weighted = jnp.dot(weights.astype(jnp.bfloat16), cached_lat, preferred_element_type=jnp.float32) + rounded_new[:, None] * new_latent.astype(jnp.float32)[None, :]
    return (weighted / weight_sum[:, None]).astype(jnp.bfloat16)

def reference(tokens, token_gain, w_query, w_down_kv, w_rope_key, latent_gain, w_key_up, w_value_up, w_out, out_gain, cache_latent, cache_rope, lengths):
    token_values = tokens.astype(jnp.float32)
    scaled = (token_values * token_gain).astype(jnp.bfloat16)
    query_heads = jnp.dot(scaled, w_query, preferred_element_type=jnp.float32).astype(jnp.bfloat16).reshape(BATCH, HEADS, NOPE + ROPE)
    latent_raw = jnp.dot(scaled, w_down_kv, preferred_element_type=jnp.float32)
    rope_raw = jnp.dot(scaled, w_rope_key, preferred_element_type=jnp.float32)
    latent = (latent_raw * lax.rsqrt(lax.optimization_barrier(jnp.mean(latent_raw * latent_raw, axis=1, keepdims=True)) + EPSILON) * latent_gain).astype(jnp.bfloat16)
    cosine, sine_table = angle_tables(lengths, ROPE)
    new_rope = rotate_half(rope_raw, cosine, sine_table).astype(jnp.bfloat16)
    query_nope = query_heads[..., :NOPE]
    query_rope = rotate_half(query_heads[..., NOPE:].astype(jnp.float32), cosine[:, None, :], sine_table[:, None, :]).astype(jnp.bfloat16)
    query_latent = jnp.einsum('bhn,hcn->bhc', query_nope.astype(jnp.float32), w_key_up.astype(jnp.float32)).astype(jnp.bfloat16)
    head_latent = lax.map(attend_one, (query_latent, query_rope, latent, new_rope, lengths, cache_latent, cache_rope))
    head_out = jnp.einsum('bhc,hcv->bhv', head_latent.astype(jnp.float32), w_value_up.astype(jnp.float32)).astype(jnp.bfloat16).reshape(BATCH, HEADS * VDIM)
    mixed_sum = jnp.dot(head_out, w_out, preferred_element_type=jnp.float32)
    out_inverse = lax.rsqrt(lax.optimization_barrier(jnp.mean(mixed_sum * mixed_sum, axis=1)) + EPSILON)[:, None]
    return (mixed_sum * out_inverse * out_gain).astype(jnp.bfloat16)
```

```python
import functools

import jax
import jax.numpy as jnp
import numpy as np
from jax import lax
from jax.experimental import pallas as pl
from jax.experimental.pallas import tpu as pltpu
from jax.sharding import PartitionSpec as P

EPSILON = 1e-06
NEGATIVE = -1e30
LANES = 128
MESH = pl.DeviceIdType.MESH
F32 = jnp.float32
BF16 = jnp.bfloat16
SIDE = 4
KV = 16
TP = 8
SEQS = 8
HEADS = 8
LATENT = 512
NOPE = 128
ROPE = 64
POS = 512
FULL = LATENT + LANES
ROWS = 4
FACTOR = (NOPE + ROPE) ** (-0.5)
MODEL = 2048


def ring_distance(d):
    return min(d % SIDE, -d % SIDE)


PLANE = sorted(
    [(a, b) for a in range(SIDE) for b in range(SIDE) if (a, b) != (0, 0)],
    key=lambda d: -(ring_distance(d[0]) + ring_distance(d[1])),
)
LINE = sorted(
    [(a, b) for a in range(SIDE) for b in range(2) if (a, b) != (0, 0)],
    key=lambda d: -(2 * ring_distance(d[0]) + d[1]),
)
EVERYWHERE = sorted(
    [
        (a, b, c, d)
        for a in range(SIDE)
        for b in range(SIDE)
        for c in range(SIDE)
        for d in range(2)
        if (a, b, c, d) != (0, 0, 0, 0)
    ],
    key=lambda d: -(2 * sum(ring_distance(i) for i in d[:3]) + d[3]),
)


def rounded(values):
    return values.astype(BF16).astype(F32)


def dot_t(a, b):
    return lax.dot_general(a, b, (((1,), (1,)), ((), ())), preferred_element_type=F32)


def dot(a, b):
    return jnp.dot(a, b, preferred_element_type=F32)


def rotated(values, cosine, signed_sine):
    half = ROPE // 2
    lane = lax.broadcasted_iota(jnp.int32, values.shape, 1)
    swapped = jnp.where(
        lane % ROPE < half,
        pltpu.roll(values, LANES - half, 1),
        pltpu.roll(values, half, 1),
    )
    return values * cosine + swapped * signed_sine


def kernel(
    lengths,
    freq_h,
    tok_h,
    tgain_h,
    wq_h,
    wd_h,
    wr_h,
    wku_h,
    cl_h,
    cr_h,
    lgain_h,
    wvu_h,
    wo_h,
    ogain_h,
    out,
    freq,
    tok,
    tgain,
    wq,
    wd,
    wr,
    wku,
    cl,
    cr,
    lgain,
    wvu,
    ogain,
    wo_all,
    wkut,
    clt,
    scaled_s,
    q_send,
    q_recv,
    lat_send,
    lat_recv,
    row_send,
    row_recv,
    ql_send,
    ql_recv,
    qm,
    qr,
    wm,
    part_send,
    part_recv,
    wv_recv,
    ho_send,
    ho_recv,
    sq_send,
    sq_recv,
    in_sem,
    ss,
    q_rs,
    lat_rs,
    row_rs,
    ql_rs,
    part_rs,
    wv_rs,
    wo_rs,
    ho_rs,
    sq_rs,
    ql_ss,
    row_ss,
    lat_ss,
):
    k = lax.axis_index("kv")
    t = lax.axis_index("tp")
    z, x = k // SIDE, k % SIDE
    y, core = t // 2, t % 2

    def load(i, a, b):
        copy = pltpu.make_async_copy(a, b, in_sem.at[i])
        copy.start()
        return copy

    half_w = NOPE + ROPE
    first = [
        load(0, tok_h, tok),
        load(1, tgain_h, tgain),
        load(2, wq_h, wq.at[pl.ds(0, half_w)]),
        load(3, wq_h.at[pl.ds(NOPE, ROPE)], wq.at[pl.ds(half_w, ROPE)]),
    ]
    load_lat = [
        load(4, wd_h, wd),
        load(5, wr_h, wr.at[pl.ds(0, ROPE)]),
        load(6, freq_h, freq),
    ]
    load_up = [load(7, wku_h, wku)]
    load_cl = [load(8, cl_h, cl)]
    load_cr = [load(9, cr_h, cr)]
    load_wvu = load(10, wvu_h, wvu)
    load_wo = load(11, wo_h, wo_all.at[t])
    load_gain = [load(12, lgain_h, lgain), load(13, ogain_h, ogain)]

    def at_plane(d):
        return ((z + d[0]) % SIDE) * SIDE + (x + d[1]) % SIDE

    def at_line(d):
        return ((y + d[0]) % SIDE) * 2 + (core + d[1]) % 2

    barrier = pltpu.get_barrier_semaphore()
    for d in PLANE:
        pl.semaphore_signal(barrier, inc=1, device_id=(at_plane(d), t), device_id_type=MESH)
    for d in LINE:
        pl.semaphore_signal(barrier, inc=1, device_id=(k, at_line(d)), device_id_type=MESH)

    def remote(src, dst, send, recv, kk, tt):
        return pltpu.make_async_remote_copy(
            src_ref=src,
            dst_ref=dst,
            send_sem=send,
            recv_sem=recv,
            device_id=(kk, tt),
            device_id_type=MESH,
        )

    def push(src, dst, send, recv, kk, tt):
        same = jnp.logical_and(kk == k, tt == t)

        @pl.when(jnp.logical_not(same))
        def _():
            remote(src, dst, send, recv, kk, tt).start()

        @pl.when(same)
        def _():
            pltpu.make_async_copy(src, dst, recv).start()

    def pushed(src, dst, send, recv, kk, tt):
        same = jnp.logical_and(kk == k, tt == t)

        @pl.when(jnp.logical_not(same))
        def _():
            remote(src, dst, send, recv, kk, tt).wait_send()

    def wait_bytes(ref, sem):
        pltpu.make_async_copy(ref, ref, sem).wait()

    with jax.named_scope("q_partial"):
        for c in first:
            c.wait()
        scaled = (tok[...].astype(F32) * tgain[...]).astype(BF16)
        query = dot_t(scaled, wq[...]).astype(BF16)
        for p in range(4):
            q_send[p] = query[16 * p : 16 * p + 16]
        mine = (x + 2 * z) % 4
        q_recv[k] = q_send[mine]
        wide = scaled.astype(F32)
        for group in range(TP):
            scaled_s[group] = wide[group * SEQS : (group + 1) * SEQS]

    with jax.named_scope("barrier"):
        pl.semaphore_wait(barrier, len(PLANE) + len(LINE))

    with jax.named_scope("send_q"):
        for d in PLANE:
            kk = at_plane(d)
            server = ((x + d[1]) + 2 * (z + d[0])) % 4
            remote(q_send.at[server], q_recv.at[k], ss.at[0], q_rs, kk, t).start()

    wv_to = ((y - z) % SIDE) * 2 + (core - x // 2) % 2
    local_wv = jnp.logical_and(z == 0, x // 2 == 0)
    with jax.named_scope("send_wv"):
        load_wvu.wait()

        @pl.when(jnp.logical_not(local_wv))
        def _():
            remote(wvu, wv_recv, ss.at[1], wv_rs, k, wv_to).start()

        @pl.when(local_wv)
        def _():
            wv_recv[...] = wvu[...]

    with jax.named_scope("lat_partial"):
        for c in load_lat:
            c.wait()
        own = scaled_s[t].astype(BF16)
        lat = dot(own, wd[...])
        wr[ROPE:, :] = jnp.zeros((LANES - ROPE, LANES), BF16)
        rope = dot_t(own, wr[...])
        for i in range(SEQS):
            lat_send[i, :, :LATENT] = lat[i : i + 1]
            lat_send[i, :, LATENT:] = rope[i : i + 1]
        lat_args = lambda i: (
            lat_send.at[i // 2],
            lat_recv.at[k],
            lat_ss.at[i],
            lat_rs.at[k],
            i,
            t,
        )

        def lat_step(i, carry):
            push(*lat_args(i))
            return carry

        lax.fori_loop(0, KV, lat_step, 0)

    with jax.named_scope("tables"):
        lane = lax.broadcasted_iota(jnp.int32, (1, LANES), 1)
        sign = jnp.where(lane % ROPE < ROPE // 2, -1.0, 1.0)
        row16 = lax.broadcasted_iota(jnp.int32, (16, LANES), 0)
        len16 = jnp.zeros((16, LANES), F32)
        for i in range(16):
            len16 = jnp.where(row16 == i, lengths[mine * 16 + i].astype(F32), len16)
        angle = len16 * freq[...]
        cos16 = jnp.cos(angle)
        sin16 = jnp.sin(angle) * sign
        seq = k // 2
        angle1 = lengths[t * SEQS + seq].astype(F32) * freq[...]
        cos1 = jnp.cos(angle1)
        sin1 = jnp.sin(angle1) * sign
        row8 = lax.broadcasted_iota(jnp.int32, (SEQS, POS), 0)
        len8 = jnp.zeros((SEQS, POS), jnp.int32)
        for b in range(SEQS):
            len8 = jnp.where(row8 == b, lengths[t * SEQS + b], len8)
        place = k * POS + lax.broadcasted_iota(jnp.int32, (SEQS, POS), 1)
        left8 = len8 - place
        load_up[0].wait()
        wkut[...] = wku[0].T

    with jax.named_scope("transpose"):
        load_cl[0].wait()
        for b in range(SEQS):
            clt[b * LATENT : (b + 1) * LATENT, :] = cl[b * POS : (b + 1) * POS, :].T

    with jax.named_scope("wait_q"):
        wait_bytes(q_recv.at[pl.ds(0, KV - 1)], q_rs)

    with jax.named_scope("key_up"):
        query = q_recv[0].astype(F32)
        for i in range(1, KV):
            query = query + q_recv[i].astype(F32)
        query = rounded(query)
        spun = rotated(query[:, NOPE:], cos16, sin16)
        up = dot(query[:, :NOPE].astype(BF16), wkut[...])
        for g in range(2):
            ql_send[g, :, :LATENT] = up[g * SEQS : (g + 1) * SEQS].astype(BF16)
            ql_send[g, :, LATENT:] = spun[g * SEQS : (g + 1) * SEQS].astype(BF16)

    def ql_all(act):
        for j, d in enumerate(((0, 1), (0, -1), (-1, 0), (0, 0))):
            for g in range(2):
                act(
                    ql_send.at[g],
                    ql_recv.at[t],
                    ql_ss.at[2 * j + g],
                    ql_rs.at[t],
                    at_plane(d),
                    2 * mine + g,
                )

    with jax.named_scope("send_ql"):
        ql_all(push)

    with jax.named_scope("send_wo"):
        load_wo.wait()
        for d in LINE:
            remote(wo_all.at[t], wo_all.at[t], ss.at[2], wo_rs, k, at_line(d)).start()

    with jax.named_scope("new_row"):
        load_gain[0].wait()
        for i in range(KV):
            wait_bytes(lat_recv.at[i], lat_rs.at[i])
        fresh = lat_recv[0]
        for i in range(1, KV):
            fresh = fresh + lat_recv[i]
        fresh_lat = fresh[:, :LATENT]
        scale = lax.rsqrt(jnp.mean(fresh_lat * fresh_lat, axis=1, keepdims=True) + EPSILON)
        row_send[:, :LATENT] = rounded(fresh_lat * scale * lgain[...])
        row_send[:, LATENT:] = rounded(rotated(fresh[:, LATENT:], cos1, sin1))
        row_args = lambda i: (
            row_send,
            row_recv.at[seq % ROWS],
            row_ss.at[i],
            row_rs.at[seq % ROWS],
            2 * (4 * (k % 2) + i) + seq // ROWS,
            t,
        )
        for i in range(4):
            push(*row_args(i))

    with jax.named_scope("masks"):
        load_cr[0].wait()
        rowp = lax.broadcasted_iota(jnp.int32, (64, LANES), 0) % SEQS
        lanep = lax.broadcasted_iota(jnp.int32, (64, LANES), 1) // ROPE
        keep = [(rowp == b).astype(F32).astype(BF16) for b in range(SEQS)]
        keep_rope = [(rowp == lanep + 2 * c).astype(F32).astype(BF16) for c in range(4)]
        left = jnp.concatenate([left8] * HEADS, axis=0)
        visible = left > 0

    with jax.named_scope("wait_ql"):
        for i in range(HEADS):
            wait_bytes(ql_recv.at[i], ql_rs.at[i])

    with jax.named_scope("scores"):
        q = jnp.concatenate([ql_recv[i].astype(F32) for i in range(HEADS)], axis=0).astype(BF16)
        for c in range(LATENT // LANES):
            piece = q[:, c * LANES : (c + 1) * LANES]
            for b in range(SEQS):
                qm[:, b * LATENT + c * LANES : b * LATENT + (c + 1) * LANES] = piece * keep[b]
        piece = q[:, LATENT:]
        for c in range(4):
            qr[:, c * LANES : (c + 1) * LANES] = piece * keep_rope[c]
        scores = (dot(qm[...], clt[...]) + dot(qr[...], cr[...])) * FACTOR
    with jax.named_scope("softmax"):
        scores = jnp.where(visible, scores, NEGATIVE)
        top = jnp.max(scores, axis=1, keepdims=True)
        weights = jnp.where(visible, jnp.exp(scores - top), 0.0)
        total = jnp.sum(weights, axis=1, keepdims=True)
        wb = weights.astype(BF16)
        for c in range(POS // LANES):
            piece = wb[:, c * LANES : (c + 1) * LANES]
            for b in range(SEQS):
                wm[:, b * POS + c * LANES : b * POS + (c + 1) * LANES] = piece * keep[b]
        lane64 = lax.broadcasted_iota(jnp.int32, (64, LANES), 1)
        stats = jnp.zeros((64, LANES), F32)
        for at, value in ((0, top), (3, total)):
            for i in range(3):
                bit = rounded(value)
                stats = jnp.where(lane64 == at + i, bit, stats)
                value = value - bit
    with jax.named_scope("attend"):
        acc = dot(wm[...], cl[...])
        for i in range(KV):
            part_send[i, :, :LATENT] = acc[i * ROWS : (i + 1) * ROWS].astype(BF16)
            part_send[i, :, LATENT:] = stats[i * ROWS : (i + 1) * ROWS].astype(BF16)

    def head_of(zz, xx):
        return ((y + zz) % SIDE) * 2 + (core + (xx % SIDE) // 2) % 2

    head = head_of(z, x)
    part = x % 2
    with jax.named_scope("send_part"):
        for d in PLANE:
            index = head_of(z + d[0], x + d[1]) * 2 + (x + d[1]) % 2
            remote(
                part_send.at[index], part_recv.at[k], ss.at[3], part_rs, at_plane(d), t
            ).start()
        part_recv[k] = part_send[head * 2 + part]

    with jax.named_scope("new_score"):
        for i in range(ROWS):
            wait_bytes(row_recv.at[i], row_rs.at[i])
        new_key = jnp.concatenate([row_recv[i] for i in range(ROWS)], axis=0)
        own_query = ql_recv[head].astype(F32)
        own_query = jnp.where(part == 0, own_query[:ROWS], own_query[ROWS:])
        new_score = jnp.sum(own_query * new_key, axis=1, keepdims=True) * FACTOR

        @pl.when(jnp.logical_not(local_wv))
        def _():
            wait_bytes(wv_recv, wv_rs)

    with jax.named_scope("wait_part"):
        wait_bytes(part_recv.at[pl.ds(0, KV - 1)], part_rs)

    with jax.named_scope("combine"):
        tops, sums = [], []
        best = new_score
        for i in range(KV):
            stats = part_recv[i, :, LATENT:].astype(F32)
            top = stats[:, 0:1] + stats[:, 1:2] + stats[:, 2:3]
            tops.append(top)
            sums.append(stats[:, 3:4] + stats[:, 4:5] + stats[:, 5:6])
            best = jnp.maximum(best, top)
        new_weight = jnp.exp(new_score - best)
        weighted = rounded(new_weight) * new_key[:, :LATENT]
        weight_sum = new_weight
        for i in range(KV):
            share = jnp.exp(tops[i] - best)
            weight_sum = weight_sum + share * sums[i]
            weighted = weighted + share * part_recv[i, :, :LATENT].astype(F32)
        hl = (weighted / weight_sum).astype(BF16)
        ho_send[...] = dot(hl, wv_recv[0]).astype(BF16)
        slot = head * 16 + t * 2 + part
        ho_recv[slot] = ho_send[...]

    with jax.named_scope("send_ho"):
        for d in EVERYWHERE:
            remote(
                ho_send, ho_recv.at[slot], ss.at[4], ho_rs, at_plane(d[:2]), at_line(d[2:])
            ).start()

    with jax.named_scope("wait_ho"):
        load_gain[1].wait()
        wait_bytes(wo_all.at[pl.ds(0, TP - 1)], wo_rs)
        wait_bytes(ho_recv.at[pl.ds(0, KV * TP - 1)], ho_rs)

    with jax.named_scope("mix"):
        mixed = None
        for h in range(HEADS):
            block = jnp.concatenate(
                [ho_recv[h * 16 + j].astype(F32) for j in range(16)], axis=0
            ).astype(BF16)
            term = dot(block, wo_all[h])
            mixed = term if mixed is None else mixed + term
        squares = jnp.sum(mixed * mixed, axis=1, keepdims=True)
        diagonal = lax.broadcasted_iota(jnp.int32, (64, LANES), 0) == lane64
        sq_send[...] = jnp.sum(jnp.where(diagonal, squares, 0.0), axis=0, keepdims=True)
        sq_recv[k] = sq_send[...]

    with jax.named_scope("send_sq"):
        for d in PLANE:
            remote(sq_send, sq_recv.at[k], ss.at[5], sq_rs, at_plane(d), t).start()
        mixed = mixed * ogain[...]

    with jax.named_scope("drain"):
        wait_bytes(q_recv.at[pl.ds(0, KV - 1)], ss.at[0])

        @pl.when(jnp.logical_not(local_wv))
        def _():
            wait_bytes(wv_recv, ss.at[1])

        wait_bytes(wo_all.at[pl.ds(0, TP - 1)], ss.at[2])
        wait_bytes(part_recv.at[pl.ds(0, KV - 1)], ss.at[3])
        wait_bytes(ho_recv.at[pl.ds(0, KV * TP - 1)], ss.at[4])
        ql_all(pushed)
        for i in range(4):
            pushed(*row_args(i))

        def lat_done(i, carry):
            pushed(*lat_args(i))
            return carry

        lax.fori_loop(0, KV, lat_done, 0)

    with jax.named_scope("wait_sq"):
        wait_bytes(sq_recv.at[pl.ds(0, KV - 1)], sq_rs)

    with jax.named_scope("finish"):
        line = sq_recv[0]
        for i in range(1, KV):
            line = line + sq_recv[i]
        squares = jnp.sum(jnp.where(diagonal, line, 0.0), axis=1, keepdims=True)
        out[...] = (mixed * lax.rsqrt(squares / MODEL + EPSILON)).astype(out.dtype)
        wait_bytes(sq_recv.at[pl.ds(0, KV - 1)], ss.at[5])


def on_device(
    tokens,
    token_gain,
    w_query,
    w_down_kv,
    w_rope_key,
    latent_gain,
    w_key_up,
    w_value_up,
    w_out,
    out_gain,
    cache_latent,
    cache_rope,
    lengths,
):
    inverse = 1.0 / 10000.0 ** (np.arange(0, ROPE, 2, dtype=np.float32) / np.float32(ROPE))
    freq = jnp.asarray(np.tile(inverse.astype(np.float32), 4)[None, :])
    arrays = [
        freq,
        tokens,
        token_gain[None, :],
        w_query.T,
        w_down_kv,
        w_rope_key.T,
        w_key_up,
        cache_latent.reshape(SEQS * POS, LATENT),
        jnp.swapaxes(cache_rope, 1, 2).reshape(SEQS * ROPE, POS),
        latent_gain[None, :],
        w_value_up,
        w_out,
        out_gain[None, :],
    ]
    dma = lambda *n: pltpu.SemaphoreType.DMA(n)
    v = lambda *shape: pltpu.VMEM(shape, BF16)
    f = lambda *shape: pltpu.VMEM(shape, F32)
    return pl.pallas_call(
        kernel,
        out_shape=jax.ShapeDtypeStruct((64, LANES), BF16),
        in_specs=[pl.BlockSpec(memory_space=pltpu.SMEM)]
        + [pl.BlockSpec(memory_space=pl.ANY)] * len(arrays),
        out_specs=pl.BlockSpec(memory_space=pltpu.VMEM),
        scratch_shapes=[
            f(1, LANES),
            v(64, LANES),
            f(1, LANES),
            v(256, LANES),
            v(LANES, LATENT),
            v(LANES, LANES),
            v(1, LATENT, NOPE),
            v(SEQS * POS, LATENT),
            v(SEQS * ROPE, POS),
            f(1, LATENT),
            v(1, LATENT, NOPE),
            f(1, LANES),
            v(TP, LANES, LANES),
            v(NOPE, LATENT),
            v(SEQS * LATENT, POS),
            f(TP, SEQS, LANES),
            v(4, 16, 256),
            v(KV, 16, 256),
            f(SEQS, 1, FULL),
            f(KV, 1, FULL),
            f(1, FULL),
            f(ROWS, 1, FULL),
            v(2, SEQS, FULL),
            v(HEADS, SEQS, FULL),
            v(64, SEQS * LATENT),
            v(64, SEQS * ROPE),
            v(64, SEQS * POS),
            v(KV, ROWS, FULL),
            v(KV, ROWS, FULL),
            v(1, LATENT, NOPE),
            v(ROWS, LANES),
            v(KV * TP, ROWS, LANES),
            f(1, LANES),
            f(KV, 1, LANES),
            dma(14),
            dma(6),
            dma(),
            dma(KV),
            dma(ROWS),
            dma(HEADS),
            dma(),
            dma(),
            dma(),
            dma(),
            dma(),
            dma(8),
            dma(4),
            dma(KV),
        ],
        compiler_params=pltpu.CompilerParams(
            collective_id=0, has_side_effects=True, vmem_limit_bytes=56 * 1024 * 1024
        ),
        name="decode",
    )(lengths, *arrays)


def solution(mesh):
    placed = (
        P(None, "kv"),
        P("kv"),
        P("kv", "tp"),
        P("kv", None),
        P("kv", None),
        P(),
        P("tp", None, None),
        P("tp", None, None),
        P("tp", "kv"),
        P("kv"),
        P("tp", "kv", None),
        P("tp", "kv", None),
        P(),
    )
    return jax.shard_map(
        on_device,
        mesh=mesh,
        in_specs=placed,
        out_specs=P(None, "kv"),
        check_vma=False,
    )
```

```python
import functools

import jax
import jax.numpy as jnp
import numpy as np
from jax import lax
from jax.experimental import pallas as pl
from jax.experimental.pallas import tpu as pltpu
from jax.sharding import PartitionSpec as P

EPSILON = 1e-06
NEGATIVE = -1e30
LANES = 128
MESH = pl.DeviceIdType.MESH
F32 = jnp.float32
BF16 = jnp.bfloat16
SIDE = 4
KV = 16
TP = 8
SEQS = 8
HEADS = 8
LATENT = 512
NOPE = 128
ROPE = 64
POS = 512
FULL = LATENT + LANES
FACTOR = (NOPE + ROPE) ** (-0.5)
MODEL = 2048


def ring_distance(d):
    return min(d % SIDE, -d % SIDE)


PLANE = sorted(
    [(a, b) for a in range(SIDE) for b in range(SIDE) if (a, b) != (0, 0)],
    key=lambda d: -(ring_distance(d[0]) + ring_distance(d[1])),
)
LINE = sorted(
    [(a, b) for a in range(SIDE) for b in range(2) if (a, b) != (0, 0)],
    key=lambda d: -(2 * ring_distance(d[0]) + d[1]),
)
NEAR = ((0, 0), (0, 1), (0, 3), (1, 0), (3, 0), (0, 2), (1, 1), (1, 3))
SERVED = sorted(
    [
        (a, b, c, d)
        for a, b in NEAR
        for c in range(SIDE)
        for d in range(2)
        if (a, b, c, d) != (0, 0, 0, 0)
    ],
    key=lambda d: -(2 * sum(ring_distance(i) for i in d[:3]) + d[3]),
)


def rounded(values):
    return values.astype(BF16).astype(F32)


def dot_t(a, b):
    return lax.dot_general(a, b, (((1,), (1,)), ((), ())), preferred_element_type=F32)


def dot(a, b):
    return jnp.dot(a, b, preferred_element_type=F32)


def rotated(values, cosine, signed_sine):
    half = ROPE // 2
    lane = lax.broadcasted_iota(jnp.int32, values.shape, 1)
    swapped = jnp.where(
        lane % ROPE < half,
        pltpu.roll(values, LANES - half, 1),
        pltpu.roll(values, half, 1),
    )
    return values * cosine + swapped * signed_sine


def kernel(
    lengths,
    freq_h,
    tok_h,
    tgain_h,
    wq_h,
    wd_h,
    wr_h,
    wku_h,
    cl_h,
    cr_h,
    lgain_h,
    wvu_h,
    wo_h,
    ogain_h,
    out,
    freq,
    tok,
    tgain,
    wq,
    wd,
    wr,
    wku,
    cl,
    cr,
    lgain,
    wvu,
    ogain,
    wo_all,
    wkut,
    clt,
    scaled_s,
    q_send,
    q_recv,
    lat_send,
    lat_recv,
    row_send,
    row_recv,
    ql_send,
    ql_recv,
    qm,
    qr,
    wm,
    part_send,
    part_recv,
    wv_recv,
    ho_send,
    ho_recv,
    sq_send,
    sq_recv,
    in_sem,
    ss,
    q_rs,
    lat_rs,
    row_rs,
    ql_rs,
    part_rs,
    wv_rs,
    wo_rs,
    ho_rs,
    sq_rs,
    ql_ss,
    row_ss,
    lat_ss,
):
    k = lax.axis_index("kv")
    t = lax.axis_index("tp")
    z, x = k // SIDE, k % SIDE
    y, core = t // 2, t % 2

    def at_plane(d):
        return ((z + d[0]) % SIDE) * SIDE + (x + d[1]) % SIDE

    def at_line(d):
        return ((y + d[0]) % SIDE) * 2 + (core + d[1]) % 2

    barrier = pltpu.get_barrier_semaphore()
    for d in PLANE:
        pl.semaphore_signal(barrier, inc=1, device_id=(at_plane(d), t), device_id_type=MESH)
    for d in LINE:
        pl.semaphore_signal(barrier, inc=1, device_id=(k, at_line(d)), device_id_type=MESH)

    def load(i, a, b):
        copy = pltpu.make_async_copy(a, b, in_sem.at[i])
        copy.start()
        return copy

    half_w = NOPE + ROPE
    first = [
        load(0, tok_h, tok),
        load(1, tgain_h, tgain),
        load(2, wq_h, wq.at[pl.ds(0, half_w)]),
        load(3, wq_h.at[pl.ds(NOPE, ROPE)], wq.at[pl.ds(half_w, ROPE)]),
    ]
    load_lat = [
        load(4, wd_h, wd),
        load(5, wr_h, wr.at[pl.ds(0, ROPE)]),
        load(6, freq_h, freq),
    ]
    load_up = [load(7, wku_h, wku)]
    load_cl = [load(8, cl_h, cl)]
    load_cr = [load(9, cr_h, cr)]
    load_wo = load(11, wo_h, wo_all.at[t])
    load_gain = [load(12, lgain_h, lgain), load(13, ogain_h, ogain)]

    def head_of(d):
        zz, xx = (z + d[0]) % SIDE, x + d[1]
        m = (zz % 2) * SIDE + (xx + 2 * (zz // 2)) % SIDE
        return ((y + m // 2) % SIDE) * 2 + (core + m % 2) % 2, m

    head, shift = head_of((0, 0))
    local_wv = shift == 0
    wvu_load = pltpu.make_async_copy(wvu_h, wvu, in_sem.at[10])

    @pl.when(local_wv)
    def _():
        pltpu.make_async_copy(wvu_h, wv_recv, wv_rs).start()

    @pl.when(jnp.logical_not(local_wv))
    def _():
        wvu_load.start()

    def remote(src, dst, send, recv, kk, tt):
        return pltpu.make_async_remote_copy(
            src_ref=src,
            dst_ref=dst,
            send_sem=send,
            recv_sem=recv,
            device_id=(kk, tt),
            device_id_type=MESH,
        )

    def push(src, dst, send, recv, kk, tt):
        same = jnp.logical_and(kk == k, tt == t)

        @pl.when(jnp.logical_not(same))
        def _():
            remote(src, dst, send, recv, kk, tt).start()

        @pl.when(same)
        def _():
            pltpu.make_async_copy(src, dst, recv).start()

    def pushed(src, dst, send, recv, kk, tt):
        same = jnp.logical_and(kk == k, tt == t)

        @pl.when(jnp.logical_not(same))
        def _():
            remote(src, dst, send, recv, kk, tt).wait_send()

    def wait_bytes(ref, sem):
        pltpu.make_async_copy(ref, ref, sem).wait()

    with jax.named_scope("q_partial"):
        for c in first:
            c.wait()
        scaled = (tok[...].astype(F32) * tgain[...]).astype(BF16)
        query = dot_t(scaled, wq[...])
        for p in range(4):
            low, high = p * SEQS, (p + 4) * SEQS
            q_send[p] = jnp.concatenate(
                [query[low : low + SEQS], query[high : high + SEQS]], axis=0
            ).astype(BF16)
        mine = (x + 2 * z) % 4
        q_recv[k] = q_send[mine]
        wide = scaled.astype(F32)
        for group in range(TP):
            scaled_s[group] = wide[group * SEQS : (group + 1) * SEQS]

    with jax.named_scope("barrier"):
        pl.semaphore_wait(barrier, len(PLANE) + len(LINE))

    with jax.named_scope("send_q"):
        for d in PLANE:
            kk = at_plane(d)
            server = ((x + d[1]) + 2 * (z + d[0])) % 4
            remote(q_send.at[server], q_recv.at[k], ss.at[0], q_rs, kk, t).start()

    wv_to = ((y + SIDE - shift // 2) % SIDE) * 2 + (core + shift % 2) % 2
    with jax.named_scope("send_wv"):

        @pl.when(jnp.logical_not(local_wv))
        def _():
            wvu_load.wait()
            remote(wvu, wv_recv, ss.at[1], wv_rs, k, wv_to).start()

    with jax.named_scope("lat_partial"):
        for c in load_lat:
            c.wait()
        own = scaled_s[t].astype(BF16)
        lat = dot(own, wd[...])
        wr[ROPE:, :] = jnp.zeros((LANES - ROPE, LANES), BF16)
        rope = dot_t(own, wr[...])
        for i in range(SEQS):
            lat_send[i, :, :LATENT] = lat[i : i + 1]
            lat_send[i, :, LATENT:] = rope[i : i + 1]
        lat_args = lambda i: (
            lat_send.at[i // 2],
            lat_recv.at[k],
            lat_ss.at[i],
            lat_rs.at[k],
            i,
            t,
        )

        def lat_step(i, carry):
            push(*lat_args(i))
            return carry

        lax.fori_loop(0, KV, lat_step, 0)

    with jax.named_scope("tables"):
        lane = lax.broadcasted_iota(jnp.int32, (1, LANES), 1)
        sign = jnp.where(lane % ROPE < ROPE // 2, -1.0, 1.0)
        row16 = lax.broadcasted_iota(jnp.int32, (16, LANES), 0)
        len16 = jnp.zeros((16, LANES), F32)
        for i in range(16):
            len16 = jnp.where(row16 == i, lengths[(mine + i // SEQS * 4) * SEQS + i % SEQS].astype(F32), len16)
        angle = len16 * freq[...]
        cos16 = jnp.cos(angle)
        sin16 = jnp.sin(angle) * sign
        seq = k // 2
        angle1 = lengths[t * SEQS + seq].astype(F32) * freq[...]
        cos1 = jnp.cos(angle1)
        sin1 = jnp.sin(angle1) * sign
        row8 = lax.broadcasted_iota(jnp.int32, (SEQS, POS), 0)
        len8 = jnp.zeros((SEQS, POS), jnp.int32)
        for b in range(SEQS):
            len8 = jnp.where(row8 == b, lengths[t * SEQS + b], len8)
        place = k * POS + lax.broadcasted_iota(jnp.int32, (SEQS, POS), 1)
        left8 = len8 - place
        load_up[0].wait()
        wkut[...] = wku[0].T

    with jax.named_scope("transpose"):
        load_cl[0].wait()
        for b in range(SEQS):
            clt[b * LATENT : (b + 1) * LATENT, :] = cl[b * POS : (b + 1) * POS, :].T

    with jax.named_scope("wait_q"):
        wait_bytes(q_recv.at[pl.ds(0, KV - 1)], q_rs)

    with jax.named_scope("key_up"):
        query = q_recv[0].astype(F32)
        for i in range(1, KV):
            query = query + q_recv[i].astype(F32)
        query = rounded(query)
        spun = rotated(query[:, NOPE:], cos16, sin16)
        up = dot(query[:, :NOPE].astype(BF16), wkut[...])
        for g in range(2):
            ql_send[g, :, :LATENT] = up[g * SEQS : (g + 1) * SEQS].astype(BF16)
            ql_send[g, :, LATENT:] = spun[g * SEQS : (g + 1) * SEQS].astype(BF16)

    def ql_all(act):
        for j, d in enumerate(((0, 1), (0, -1), (-1, 0), (0, 0))):
            for g in range(2):
                act(
                    ql_send.at[g],
                    ql_recv.at[t],
                    ql_ss.at[2 * j + g],
                    ql_rs.at[t],
                    at_plane(d),
                    mine + 4 * g,
                )

    with jax.named_scope("send_ql"):
        ql_all(push)

    with jax.named_scope("new_row"):
        load_gain[0].wait()
        for i in range(KV):
            wait_bytes(lat_recv.at[i], lat_rs.at[i])
        fresh = lat_recv[0]
        for i in range(1, KV):
            fresh = fresh + lat_recv[i]
        fresh_lat = fresh[:, :LATENT]
        scale = lax.rsqrt(jnp.mean(fresh_lat * fresh_lat, axis=1, keepdims=True) + EPSILON)
        row_send[:, :LATENT] = rounded(fresh_lat * scale * lgain[...])
        row_send[:, LATENT:] = rounded(rotated(fresh[:, LATENT:], cos1, sin1))
        row_args = lambda i: (
            row_send,
            row_recv.at[seq],
            row_ss.at[i],
            row_rs.at[seq],
            k % 2 + 2 * i,
            t,
        )
        for i in range(SEQS):
            push(*row_args(i))

    with jax.named_scope("masks"):
        load_cr[0].wait()
        rowp = lax.broadcasted_iota(jnp.int32, (64, LANES), 0) % SEQS
        lanep = lax.broadcasted_iota(jnp.int32, (64, LANES), 1) // ROPE
        keep = [(rowp == b).astype(F32).astype(BF16) for b in range(SEQS)]
        keep_rope = [(rowp == lanep + 2 * c).astype(F32).astype(BF16) for c in range(4)]
        left = jnp.concatenate([left8] * HEADS, axis=0)
        visible = left > 0

    with jax.named_scope("wait_ql"):
        for i in range(HEADS):
            wait_bytes(ql_recv.at[i], ql_rs.at[i])

    with jax.named_scope("send_wo"):
        load_wo.wait()
        for d in LINE:
            remote(wo_all.at[t], wo_all.at[t], ss.at[2], wo_rs, k, at_line(d)).start()

    with jax.named_scope("scores"):
        q = jnp.concatenate([ql_recv[i].astype(F32) for i in range(HEADS)], axis=0).astype(BF16)
        for c in range(LATENT // LANES):
            piece = q[:, c * LANES : (c + 1) * LANES]
            for b in range(SEQS):
                qm[:, b * LATENT + c * LANES : b * LATENT + (c + 1) * LANES] = piece * keep[b]
        piece = q[:, LATENT:]
        for c in range(4):
            qr[:, c * LANES : (c + 1) * LANES] = piece * keep_rope[c]
        scores = (dot(qm[...], clt[...]) + dot(qr[...], cr[...])) * FACTOR
    with jax.named_scope("softmax"):
        scores = jnp.where(visible, scores, NEGATIVE)
        top = jnp.max(scores, axis=1, keepdims=True)
        weights = jnp.where(visible, jnp.exp(scores - top), 0.0)
        total = jnp.sum(weights, axis=1, keepdims=True)
        wb = weights.astype(BF16)
        for c in range(POS // LANES):
            piece = wb[:, c * LANES : (c + 1) * LANES]
            for b in range(SEQS):
                wm[:, b * POS + c * LANES : b * POS + (c + 1) * LANES] = piece * keep[b]
        lane64 = lax.broadcasted_iota(jnp.int32, (64, LANES), 1)
        stats = jnp.zeros((64, LANES), F32)
        for at, value in ((0, top), (3, total)):
            for i in range(3):
                bit = rounded(value)
                stats = jnp.where(lane64 == at + i, bit, stats)
                value = value - bit
    with jax.named_scope("attend"):
        acc = dot(wm[...], cl[...])
        for i in range(HEADS):
            part_send[i, :, :LATENT] = acc[i * SEQS : (i + 1) * SEQS].astype(BF16)
            part_send[i, :, LATENT:] = stats[i * SEQS : (i + 1) * SEQS].astype(BF16)

    with jax.named_scope("send_part"):
        for d in PLANE:
            remote(
                part_send.at[head_of(d)[0]], part_recv.at[k], ss.at[3], part_rs, at_plane(d), t
            ).start()
        part_recv[k] = part_send[head]

    with jax.named_scope("new_score"):
        for i in range(SEQS):
            wait_bytes(row_recv.at[i], row_rs.at[i])
        new_key = jnp.concatenate([row_recv[i] for i in range(SEQS)], axis=0)
        own_query = ql_recv[head].astype(F32)
        new_score = jnp.sum(own_query * new_key, axis=1, keepdims=True) * FACTOR
        wait_bytes(wv_recv, wv_rs)

    with jax.named_scope("wait_part"):
        wait_bytes(part_recv.at[pl.ds(0, KV - 1)], part_rs)

    with jax.named_scope("combine"):
        tops, sums = [], []
        best = new_score
        for i in range(KV):
            stats = part_recv[i, :, LATENT:].astype(F32)
            top = stats[:, 0:1] + stats[:, 1:2] + stats[:, 2:3]
            tops.append(top)
            sums.append(stats[:, 3:4] + stats[:, 4:5] + stats[:, 5:6])
            best = jnp.maximum(best, top)
        new_weight = jnp.exp(new_score - best)
        weighted = rounded(new_weight) * new_key[:, :LATENT]
        weight_sum = new_weight
        for i in range(KV):
            share = jnp.exp(tops[i] - best)
            weight_sum = weight_sum + share * sums[i]
            weighted = weighted + share * part_recv[i, :, :LATENT].astype(F32)
        hl = (weighted / weight_sum).astype(BF16)
        ho_send[...] = dot(hl, wv_recv[0]).astype(BF16)
        slot = head * TP + t
        ho_recv[slot] = ho_send[...]

    with jax.named_scope("send_ho"):
        for d in SERVED:
            remote(
                ho_send, ho_recv.at[slot], ss.at[4], ho_rs, at_plane(d[:2]), at_line(d[2:])
            ).start()

    with jax.named_scope("wait_ho"):
        load_gain[1].wait()
        wait_bytes(wo_all.at[pl.ds(0, TP - 1)], wo_rs)
        wait_bytes(ho_recv.at[pl.ds(0, HEADS * TP - 1)], ho_rs)

    with jax.named_scope("mix"):
        mixed = None
        for h in range(HEADS):
            block = jnp.concatenate(
                [ho_recv[h * TP + j].astype(F32) for j in range(TP)], axis=0
            ).astype(BF16)
            term = dot(block, wo_all[h])
            mixed = term if mixed is None else mixed + term
        squares = jnp.sum(mixed * mixed, axis=1, keepdims=True)
        diagonal = lax.broadcasted_iota(jnp.int32, (64, LANES), 0) == lane64
        sq_send[...] = jnp.sum(jnp.where(diagonal, squares, 0.0), axis=0, keepdims=True)
        sq_recv[k] = sq_send[...]

    with jax.named_scope("send_sq"):
        for d in PLANE:
            remote(sq_send, sq_recv.at[k], ss.at[5], sq_rs, at_plane(d), t).start()
        mixed = mixed * ogain[...]

    with jax.named_scope("drain"):
        wait_bytes(q_recv.at[pl.ds(0, KV - 1)], ss.at[0])

        @pl.when(jnp.logical_not(local_wv))
        def _():
            wait_bytes(wv_recv, ss.at[1])

        wait_bytes(wo_all.at[pl.ds(0, TP - 1)], ss.at[2])
        wait_bytes(part_recv.at[pl.ds(0, KV - 1)], ss.at[3])
        wait_bytes(ho_recv.at[pl.ds(0, HEADS * TP - 1)], ss.at[4])
        ql_all(pushed)
        for i in range(SEQS):
            pushed(*row_args(i))

        def lat_done(i, carry):
            pushed(*lat_args(i))
            return carry

        lax.fori_loop(0, KV, lat_done, 0)

    with jax.named_scope("wait_sq"):
        wait_bytes(sq_recv.at[pl.ds(0, KV - 1)], sq_rs)

    with jax.named_scope("finish"):
        line = sq_recv[0]
        for i in range(1, KV):
            line = line + sq_recv[i]
        squares = jnp.sum(jnp.where(diagonal, line, 0.0), axis=1, keepdims=True)
        out[...] = (mixed * lax.rsqrt(squares / MODEL + EPSILON)).astype(out.dtype)
        wait_bytes(sq_recv.at[pl.ds(0, KV - 1)], ss.at[5])


def on_device(
    tokens,
    token_gain,
    w_query,
    w_down_kv,
    w_rope_key,
    latent_gain,
    w_key_up,
    w_value_up,
    w_out,
    out_gain,
    cache_latent,
    cache_rope,
    lengths,
):
    inverse = 1.0 / 10000.0 ** (np.arange(0, ROPE, 2, dtype=np.float32) / np.float32(ROPE))
    freq = jnp.asarray(np.tile(inverse.astype(np.float32), 4)[None, :])
    arrays = [
        freq,
        tokens,
        token_gain[None, :],
        w_query.T,
        w_down_kv,
        w_rope_key.T,
        w_key_up,
        cache_latent.reshape(SEQS * POS, LATENT),
        jnp.swapaxes(cache_rope, 1, 2).reshape(SEQS * ROPE, POS),
        latent_gain[None, :],
        w_value_up,
        w_out,
        out_gain[None, :],
    ]
    dma = lambda *n: pltpu.SemaphoreType.DMA(n)
    v = lambda *shape: pltpu.VMEM(shape, BF16)
    f = lambda *shape: pltpu.VMEM(shape, F32)
    return pl.pallas_call(
        kernel,
        out_shape=pltpu.VMEM((64, LANES), BF16),
        in_specs=[pl.BlockSpec(memory_space=pltpu.SMEM)]
        + [pl.BlockSpec(memory_space=pl.ANY)] * len(arrays),
        out_specs=pl.BlockSpec(memory_space=pltpu.VMEM),
        scratch_shapes=[
            f(1, LANES),
            v(64, LANES),
            f(1, LANES),
            v(256, LANES),
            v(LANES, LATENT),
            v(LANES, LANES),
            v(1, LATENT, NOPE),
            v(SEQS * POS, LATENT),
            v(SEQS * ROPE, POS),
            f(1, LATENT),
            v(1, LATENT, NOPE),
            f(1, LANES),
            v(TP, LANES, LANES),
            v(NOPE, LATENT),
            v(SEQS * LATENT, POS),
            f(TP, SEQS, LANES),
            v(4, 16, 256),
            v(KV, 16, 256),
            f(SEQS, 1, FULL),
            f(KV, 1, FULL),
            f(1, FULL),
            f(SEQS, 1, FULL),
            v(2, SEQS, FULL),
            v(HEADS, SEQS, FULL),
            v(64, SEQS * LATENT),
            v(64, SEQS * ROPE),
            v(64, SEQS * POS),
            v(HEADS, SEQS, FULL),
            v(KV, SEQS, FULL),
            v(1, LATENT, NOPE),
            v(SEQS, LANES),
            v(HEADS * TP, SEQS, LANES),
            f(1, LANES),
            f(KV, 1, LANES),
            dma(14),
            dma(6),
            dma(),
            dma(KV),
            dma(SEQS),
            dma(HEADS),
            dma(),
            dma(),
            dma(),
            dma(),
            dma(),
            dma(8),
            dma(8),
            dma(KV),
        ],
        compiler_params=pltpu.CompilerParams(
            collective_id=0, has_side_effects=True, vmem_limit_bytes=56 * 1024 * 1024
        ),
        name="decode",
    )(lengths, *arrays)


def solution(mesh):
    placed = (
        P(None, "kv"),
        P("kv"),
        P("kv", "tp"),
        P("kv", None),
        P("kv", None),
        P(),
        P("tp", None, None),
        P("tp", None, None),
        P("tp", "kv"),
        P("kv"),
        P("tp", "kv", None),
        P("tp", "kv", None),
        P(),
    )
    return jax.shard_map(
        on_device,
        mesh=mesh,
        in_specs=placed,
        out_specs=P(None, "kv"),
        check_vma=False,
    )
```
